32 devices in a mesh: kv: 16 (over z, y, x), tp: 2 (over core).
Axes of the slice: x: 2, y: 2, z: 4, core: 2. Of those that a mesh axis runs over, the one named last changes fastest.
Arguments:
- tokens: bfloat16 [64, 4096], P(None, 'kv'), may hold values from -12 to 12
- mix_gain: float32 [4096], P('kv'), may hold values from 0.1 to 1.9
- w_query: bfloat16 [4096, 2048], P('kv', 'tp'), may hold values from -0.09375 to 0.09375
- w_key: bfloat16 [4096, 2048], P('kv', 'tp'), may hold values from -0.09375 to 0.09375
- w_value: bfloat16 [4096, 2048], P('kv', 'tp'), may hold values from -0.09375 to 0.09375
- w_gate: bfloat16 [4096, 2048], P('kv', 'tp'), may hold values from -0.09375 to 0.09375
- w_beta: bfloat16 [4096, 16], P('kv', 'tp'), may hold values from -0.09375 to 0.09375
- w_decay: bfloat16 [4096, 16], P('kv', 'tp'), may hold values from -0.09375 to 0.09375
- decay_rate: float32 [16], P('tp'), may hold values from 0.05 to 3
- head_gain: float32 [128], replicated, may hold values from 0.1 to 1.9
- state: float32 [64, 16, 128, 128], P('kv', 'tp'), may hold values from -1.2 to 1.2
- w_out: bfloat16 [2048, 4096], P('tp', 'kv'), may hold values from -0.25 to 0.25
- mlp_gain: float32 [4096], P('kv'), may hold values from 0.1 to 1.9
- w_up: bfloat16 [4096, 16384], P('kv', 'tp'), may hold values from -0.09375 to 0.09375
- w_down: bfloat16 [16384, 4096], P('tp', 'kv'), may hold values from -0.046875 to 0.046875
Outputs:
- layer_out: bfloat16 [64, 4096], P(None, 'kv')
- new_state: float32 [64, 16, 128, 128], P('kv', 'tp')
The draws below stay inside these ranges and needn't reach their ends.
All inputs are finite; a program needn't handle non-finite values.
Results may differ from the reference program's by a relative error of at most 0.017.
Values may be sent and summed in bfloat16 or wider, within the bound.
A program may use at most 64 MiB of HBM per device.

```python
import math
import jax
import jax.numpy as jnp
from jax import lax

D = 4096
HEADS = 16
HEAD_DIM = 128
FF = 16384
ROWS = 64
N_TP = 2


def draw_tokens(key, part):
    columns = jnp.arange(D, dtype=jnp.float32) / D
    base = jnp.clip(jax.random.normal(key, (ROWS, D), jnp.float32), -6.0, 6.0)
    values = base * (0.5 * 4.0 ** columns)
    return values.astype(jnp.bfloat16)


def steps_of(own_key, shape, cuts, smallest, high):
    gain, own = 1.0, jax.random.fold_in(own_key, 6)
    for position, parts in cuts:
        draws = jnp.exp(jax.random.uniform(jax.random.fold_in(own, position), (parts,), jnp.float32, smallest / len(cuts), high / len(cuts)))
        gain = gain * jnp.repeat(draws, shape[position] // parts).reshape([-1 if axis == position else 1 for axis in range(len(shape))])
    return gain


def noise(key, extent, scale, limit, cuts=(), held_as=jnp.bfloat16):
    gain = steps_of(key, extent, cuts, -0.22, 0.18) if cuts else 1.0
    drawn = jax.random.normal(key, extent, jnp.float32) * scale * gain
    return jnp.minimum(jnp.maximum(drawn, -limit), limit).astype(held_as)


def setup_inputs(seed: int = 0) -> dict:
    splits = jax.random.split(jax.random.key(seed), 16)
    return {
        "tokens": draw_tokens(jax.random.fold_in(splits[15], 71), 0),
        "mix_gain": jnp.clip(1.0 + 0.18 * jax.random.normal(splits[1], (D,), jnp.float32), 0.1, 1.9),
        "w_query": noise(splits[2], (D, HEADS * HEAD_DIM), D ** -0.5, 0.09375, ((0, 16), (1, 2))),
        "w_key": noise(splits[3], (D, HEADS * HEAD_DIM), D ** -0.5, 0.09375, ((0, 16), (1, 2))),
        "w_value": noise(splits[4], (D, HEADS * HEAD_DIM), D ** -0.5, 0.09375, ((0, 16), (1, 2))),
        "w_gate": noise(splits[5], (D, HEADS * HEAD_DIM), D ** -0.5, 0.09375, ((0, 16), (1, 2))),
        "w_beta": noise(splits[6], (D, HEADS), D ** -0.5, 0.09375, ((0, 16), (1, 2))),
        "w_decay": noise(splits[7], (D, HEADS), D ** -0.5, 0.09375, ((0, 16), (1, 2))),
        "decay_rate": jnp.clip(jnp.exp(math.log(3.0) - 4.0943445 * jax.random.uniform(splits[8], (HEADS,), jnp.float32) ** steps_of(splits[8], (HEADS,), ((0, 2),), -0.2, 0.2)), 0.05, 3.0),
        "head_gain": jnp.clip(1.0 + 0.18 * jax.random.normal(splits[9], (HEAD_DIM,), jnp.float32), 0.1, 1.9),
        "state": noise(splits[10], (ROWS, HEADS, HEAD_DIM, HEAD_DIM), 0.2, 1.2, ((0, 16), (1, 2)), jnp.float32),
        "w_out": noise(splits[11], (HEADS * HEAD_DIM, D), (HEADS * HEAD_DIM // 4) ** -0.5, 0.25, ((0, 2), (1, 16))),
        "mlp_gain": jnp.clip(1.0 + 0.18 * jax.random.normal(splits[12], (D,), jnp.float32), 0.1, 1.9),
        "w_up": noise(splits[13], (D, FF), D ** -0.5, 0.09375, ((0, 16), (1, 2))),
        "w_down": noise(splits[14], (FF, D), FF ** -0.5, 0.046875, ((0, 2), (1, 16))),
    }


norm_eps = 1e-06

def rms_scale(values):
    return lax.rsqrt(lax.optimization_barrier(jnp.mean(values * values, axis=-1, keepdims=True)) + norm_eps)

def delta_update(query_pre, key_pre, value_pre, gate_pre, beta_pre, decay_pre, decay_rate, head_gain, state):
    f32 = jnp.float32
    query = jax.nn.silu(query_pre)
    query = query * lax.rsqrt(lax.optimization_barrier(jnp.sum(query * query, axis=-1, keepdims=True)) + norm_eps) * query.shape[-1] ** (-0.5)
    keyed = jax.nn.silu(key_pre)
    keyed = keyed * lax.rsqrt(lax.optimization_barrier(jnp.sum(keyed * keyed, axis=-1, keepdims=True)) + norm_eps)
    valued = jax.nn.silu(value_pre)
    beta = jax.nn.sigmoid(beta_pre)
    decay = jnp.exp(-decay_rate.astype(f32) * jax.nn.softplus(decay_pre))
    recalled = jnp.einsum('bhk,bhkv->bhv', keyed, state, precision=lax.Precision.HIGHEST)
    corrected = state - beta[:, :, None, None] * keyed[:, :, :, None] * recalled[:, :, None, :]
    new_state = decay[:, :, None, None] * corrected + beta[:, :, None, None] * keyed[:, :, :, None] * valued[:, :, None, :]
    read = jnp.einsum('bhkv,bhk->bhv', new_state, query, precision=lax.Precision.HIGHEST)
    mixed = read * rms_scale(read) * head_gain.astype(f32) * jax.nn.silu(gate_pre)
    return (mixed, new_state)

def reference(tokens, mix_gain, w_query, w_key, w_value, w_gate, w_beta, w_decay, decay_rate, head_gain, state, w_out, mlp_gain, w_up, w_down):
    f32 = jnp.float32
    bf16 = jnp.bfloat16
    rows = tokens.shape[0]
    tok32 = tokens.astype(f32)
    scale = rms_scale(tok32)
    gained = (tok32 * mix_gain.astype(f32)).astype(bf16)

    def project(weight):
        return jnp.dot(gained, weight, preferred_element_type=f32) * scale

    def heads_view(values):
        return values.reshape(rows, HEADS, HEAD_DIM)
    mixed, new_state = delta_update(heads_view(project(w_query)), heads_view(project(w_key)), heads_view(project(w_value)), heads_view(project(w_gate)), project(w_beta), project(w_decay), decay_rate, head_gain, state)
    mixed = mixed.reshape(rows, HEADS * HEAD_DIM).astype(bf16)
    group = HEADS * HEAD_DIM // N_TP
    attended = jnp.zeros((rows, D), f32)
    for index in range(N_TP):
        term = jnp.dot(mixed[:, index * group:(index + 1) * group], w_out[index * group:(index + 1) * group], preferred_element_type=f32)
        attended = attended + lax.optimization_barrier(term.astype(bf16)).astype(f32)
    residual = lax.optimization_barrier((tok32 + attended).astype(bf16)).astype(f32)
    scale_mid = rms_scale(residual)
    gained_mid = (residual * mlp_gain.astype(f32)).astype(bf16)
    up_pre = jnp.dot(gained_mid, w_up, preferred_element_type=f32) * scale_mid
    hidden = jnp.square(jax.nn.relu(up_pre)).astype(bf16)
    width = FF // N_TP
    mixer = jnp.zeros((rows, D), f32)
    for index in range(N_TP):
        term = jnp.dot(hidden[:, index * width:(index + 1) * width], w_down[index * width:(index + 1) * width], preferred_element_type=f32)
        mixer = mixer + lax.optimization_barrier(term.astype(bf16)).astype(f32)
    layer_out = (residual + mixer).astype(bf16)
    return (layer_out, new_state)
```

```python
import functools

import jax
import jax.numpy as jnp
from jax import lax
from jax.experimental import pallas as pl
from jax.experimental.pallas import tpu as pltpu
from jax.sharding import PartitionSpec as P


norm_eps = 1e-06


def rms_scale(values):
    return lax.rsqrt(jnp.mean(values * values, axis=-1, keepdims=True) + norm_eps)


def delta_update(
    query_pre, key_pre, value_pre, gate_pre, beta_pre, decay_pre, decay_rate, head_gain, state
):
    query = jax.nn.silu(query_pre)
    query = (
        query
        * lax.rsqrt(jnp.sum(query * query, axis=-1, keepdims=True) + norm_eps)
        * query.shape[-1] ** (-0.5)
    )
    keyed = jax.nn.silu(key_pre)
    keyed = keyed * lax.rsqrt(jnp.sum(keyed * keyed, axis=-1, keepdims=True) + norm_eps)
    valued = jax.nn.silu(value_pre)
    beta = jax.nn.sigmoid(beta_pre)
    decay = jnp.exp(-decay_rate * jax.nn.softplus(decay_pre))
    recalled = jnp.einsum("bhk,bhkv->bhv", keyed, state, precision=lax.Precision.HIGHEST)
    corrected = state - beta[:, :, None, None] * keyed[:, :, :, None] * recalled[:, :, None, :]
    new_state = (
        decay[:, :, None, None] * corrected
        + beta[:, :, None, None] * keyed[:, :, :, None] * valued[:, :, None, :]
    )
    read = jnp.einsum("bhkv,bhk->bhv", new_state, query, precision=lax.Precision.HIGHEST)
    mixed = read * rms_scale(read) * head_gain * jax.nn.silu(gate_pre)
    return (mixed, new_state)


def body(
    tokens,
    mix_gain,
    w_query,
    w_key,
    w_value,
    w_gate,
    w_beta,
    w_decay,
    decay_rate,
    head_gain,
    state,
    w_out,
    mlp_gain,
    w_up,
    w_down,
):
    f32 = jnp.float32
    bf16 = jnp.bfloat16
    local_rows = state.shape[0]
    heads_here = state.shape[1]
    head_size = state.shape[2]
    offset = lax.axis_index("kv") * local_rows
    D = tokens.shape[1] * lax.axis_size("kv")
    tok32 = tokens.astype(f32)
    squares = jnp.sum(tok32 * tok32, axis=1)
    gained = (tok32 * mix_gain).astype(bf16)
    joined = jnp.concatenate([w_query, w_key, w_value, w_gate], axis=1)
    rate_weights = jnp.concatenate([w_beta, w_decay], axis=1)
    main_term = jnp.dot(gained, joined, preferred_element_type=f32)
    rate_term = jnp.dot(gained, rate_weights, preferred_element_type=f32)
    energy_all = lax.psum(squares, "kv")
    main_part, rate_part = (
        lax.psum_scatter(main_term, "kv", scatter_dimension=0, tiled=True),
        lax.psum_scatter(rate_term, "kv", scatter_dimension=0, tiled=True),
    )
    energy = lax.dynamic_slice_in_dim(energy_all, offset, local_rows)
    scale = lax.rsqrt(energy / D + norm_eps)[:, None]
    main_part = (main_part * scale).reshape(local_rows, 4, heads_here, head_size)
    rate_part = rate_part * scale
    mixed, new_state = delta_update(
        main_part[:, 0],
        main_part[:, 1],
        main_part[:, 2],
        main_part[:, 3],
        rate_part[:, :heads_here],
        rate_part[:, heads_here:],
        decay_rate,
        head_gain,
        state,
    )
    mixed = mixed.reshape(local_rows, heads_here * head_size).astype(bf16)
    head_term = jnp.dot(
        lax.all_gather(mixed, "kv", axis=0, tiled=True), w_out, preferred_element_type=f32
    )
    attended = lax.psum(head_term.astype(jnp.bfloat16), "tp").astype(jnp.float32)
    residual = lax.optimization_barrier((tok32 + attended).astype(bf16)).astype(f32)
    squares_mid = jnp.sum(residual * residual, axis=1)
    gained_mid = (residual * mlp_gain).astype(bf16)
    up_term = jnp.dot(gained_mid, w_up, preferred_element_type=f32)
    up_part, energy_mid = lax.psum((up_term, squares_mid), "kv")
    scaled = up_part * lax.rsqrt(energy_mid / D + norm_eps)[:, None]
    down_term = jnp.dot(
        jnp.square(jax.nn.relu(scaled)).astype(bf16), w_down, preferred_element_type=f32
    )
    mixer = lax.psum(down_term.astype(jnp.bfloat16), "tp").astype(jnp.float32)
    layer_out = (residual + mixer).astype(bf16)
    return (layer_out, new_state)


MESH = pl.DeviceIdType.MESH
f32 = jnp.float32
bf16 = jnp.bfloat16


def inner_size(n):
    size = 1
    while size * size < n:
        size *= 2
    return size


def tiles(n, n_tp, inner, *args):
    tokens, state, w_up = args[0], args[10], args[13]
    rows, width = tokens.shape
    local, heads, size, _ = state.shape
    pairs = local * heads
    return (
        inner == 4
        and n_tp > 1
        and n % inner == 0
        and rows == n * local
        and width % 128 == 0
        and size == 128
        and heads == 8
        and pairs % 16 == 0
        and 128 % (2 * pairs) == 0
        and 128 % rows == 0
        and (rows // inner) % 16 == 0
        and w_up.shape[1] % (n * 128) == 0
        and n // inner > 1
    )


def remote(src, dst, send, recv, device):
    return pltpu.make_async_remote_copy(
        src_ref=src,
        dst_ref=dst,
        send_sem=send,
        recv_sem=recv,
        device_id=device,
        device_id_type=MESH,
    )


def kernel(
    n,
    n_tp,
    inner,
    tokens_h,
    mix_gain_h,
    w_query,
    w_key,
    w_value,
    w_gate,
    w_beta_h,
    w_decay_h,
    decay_rate_h,
    head_gain_h,
    state,
    w_out,
    mlp_gain_h,
    w_up,
    w_down,
    out,
    new_state,
    tokens,
    mix_gain,
    w_beta,
    w_decay,
    decay_rate,
    head_gain,
    mlp_gain,
    wp_v,
    state_v,
    w_out_v,
    w_up_v,
    w_down_v,
    a1,
    a1r,
    summed,
    a2,
    a2r,
    r1,
    r1r,
    rsum,
    r2,
    r2r,
    read_v,
    mix_v,
    mix_f,
    t1,
    u1,
    u1r,
    u2,
    u2r,
    en,
    hid,
    t2,
    small_sem,
    load_sem,
    state_sem,
    a1_s,
    a1_r,
    r1_s,
    r1_r,
    a2_s,
    a2_r,
    r2_s,
    r2_r,
    mx_s,
    mx_r,
    t1_s,
    t1_r,
    u1_s,
    u1_r,
    u2_s,
    u2_r,
    en_s,
    en_r,
    hz_s,
    hz_r,
    hp_s,
    hp_r,
    t2_s,
    t2_r,
):
    outer = n // inner
    rows, width = tokens.shape
    total_width = n * width
    local, heads, size, _ = state.shape
    pairs = local * heads
    group = rows // inner
    span = w_up.shape[1] // n
    me = lax.axis_index("kv")
    tp = lax.axis_index("tp")
    ours = lax.rem(me, inner)
    deep = me // inner
    sent = []

    def start(copy):
        copy.start()
        sent.append(copy)
        return copy

    def plane_peer(k):
        spot = lax.rem(ours + k, inner)
        return spot, {"kv": deep * inner + spot}

    def deep_peer(k):
        spot = lax.rem(deep + k, outer)
        return spot, {"kv": spot * inner + ours}

    small = []
    pairs_of = (
        (tokens_h, tokens),
        (mix_gain_h, mix_gain),
        (w_beta_h, w_beta),
        (w_decay_h, w_decay),
        (decay_rate_h, decay_rate),
        (head_gain_h, head_gain),
        (mlp_gain_h, mlp_gain),
    )
    for c, (src, dst) in enumerate(pairs_of):
        small.append(pltpu.make_async_copy(src, dst, small_sem.at[c]))
        small[-1].start()
    loads = []
    for c, ref in enumerate((w_query, w_key, w_value, w_gate)):
        loads.append(pltpu.make_async_copy(ref, wp_v.at[c], load_sem.at[c]))
    load_state = pltpu.make_async_copy(state, state_v, state_sem)
    load_out = pltpu.make_async_copy(w_out, w_out_v, load_sem.at[4])
    load_up = pltpu.make_async_copy(w_up, w_up_v, load_sem.at[5])
    load_down = pltpu.make_async_copy(w_down, w_down_v, load_sem.at[6])
    for copy in loads:
        copy.start()

    barrier = pltpu.get_barrier_semaphore()
    for k in range(1, outer):
        pl.semaphore_signal(
            barrier, inc=1, device_id=deep_peer(k)[1], device_id_type=MESH
        )
    for k in range(1, inner):
        pl.semaphore_signal(
            barrier, inc=1, device_id=plane_peer(k)[1], device_id_type=MESH
        )
    for k in range(1, n_tp):
        pl.semaphore_signal(
            barrier, inc=1, device_id={"tp": lax.rem(tp + k, n_tp)}, device_id_type=MESH
        )

    to_row = lax.broadcasted_iota(jnp.int32, (rows, rows), 0)
    from_row = lax.broadcasted_iota(jnp.int32, (rows, rows), 1)
    chosen = jnp.zeros((rows, rows), f32)
    for p in range(inner):
        for z in range(outer):
            begin = (p * outer + z) * local
            shift = begin - (z * inner + p) * local
            hit = (to_row - from_row == shift) & (to_row >= begin) & (to_row < begin + local)
            chosen = jnp.where(hit, 1.0, chosen)
    for copy in small:
        copy.wait()
    for copy in [load_state, load_out, load_up, load_down]:
        copy.start()
    tok32 = tokens[...].astype(f32)
    moved = jnp.dot(chosen.astype(bf16), tokens[...], preferred_element_type=f32)
    gained = (moved * mix_gain[...]).astype(bf16)
    lane = lax.broadcasted_iota(jnp.int32, (heads, 128), 1)
    sub = lax.broadcasted_iota(jnp.int32, (heads, 128), 0)
    rate_weights = jnp.concatenate(
        [
            w_beta[...].astype(f32),
            w_decay[...].astype(f32),
            jnp.zeros((128 - 2 * heads, width), f32),
        ],
        axis=0,
    ).astype(bf16)
    rate = lax.dot_general(
        gained, rate_weights, (((1,), (1,)), ((), ())), preferred_element_type=f32
    )
    energy_col = jnp.sum(moved * moved, axis=1, keepdims=True)
    lanes = lax.broadcasted_iota(jnp.int32, (rows, 128), 1)
    rate = rate + jnp.where(lanes == 2 * heads, energy_col, 0.0)
    for p in range(inner):
        r1[p] = rate[p * group : (p + 1) * group]

    pl.semaphore_wait(barrier, outer - 1 + inner - 1 + n_tp - 1)

    first = {}
    for c in range(4):
        loads[c].wait()
        term = jnp.dot(gained, wp_v[c], preferred_element_type=f32).astype(bf16)
        for p in range(inner):
            a1[c, p] = term[p * group : (p + 1) * group]
        for k in range(1, inner):
            spot, device = plane_peer(k)
            first[c, k] = start(
                remote(a1.at[c, spot], a1r.at[c, k], a1_s.at[c, k], a1_r.at[c, k], device)
            )
        if c == 0:
            for k in range(1, inner):
                spot, device = plane_peer(k)
                first["r", k] = start(
                    remote(r1.at[spot], r1r.at[k], r1_s.at[k], r1_r.at[k], device)
                )

    second = {}
    for c in range(4):
        total = a1[c, ours].astype(f32)
        for k in range(1, inner):
            first[c, k].wait_recv()
            total = total + a1r[c, k].astype(f32)
        base = c * group * heads
        for h in range(heads):
            summed[pl.ds(base + h, group, stride=heads), :] = total[
                :, h * size : (h + 1) * size
            ]
        for z in range(outer):
            a2[c, z] = summed[pl.ds(base + z * pairs, pairs), :].astype(bf16)
        for k in range(1, outer):
            spot, device = deep_peer(k)
            second[c, k] = start(
                remote(a2.at[c, spot], a2r.at[c, k], a2_s.at[c, k], a2_r.at[c, k], device)
            )
        if c == 0:
            total = r1[ours]
            for k in range(1, inner):
                first["r", k].wait_recv()
                total = total + r1r[k]
            rsum[...] = total
            r2[...] = jnp.zeros(r2.shape, f32)
            for z in range(outer):
                r2[z, 0:local, :] = rsum[z * local : (z + 1) * local, :]
            for k in range(1, outer):
                spot, device = deep_peer(k)
                second["r", k] = start(
                    remote(r2.at[spot], r2r.at[k], r2_s.at[k], r2_r.at[k], device)
                )

    rate = r2[deep]
    for k in range(1, outer):
        second["r", k].wait_recv()
        rate = rate + r2r[k]

    def column(r, first_lane, step):
        row = jnp.broadcast_to(rate[r : r + 1, :], (heads, 128))
        return jnp.sum(
            jnp.where(lane == first_lane + step * sub, row, 0.0), axis=1, keepdims=True
        )

    def columns(first_lane, step):
        return jnp.concatenate([column(r, first_lane, step) for r in range(local)], axis=0)

    scale = lax.rsqrt(columns(2 * heads, 0) / total_width + norm_eps)
    beta = jax.nn.sigmoid(columns(0, 1) * scale)
    decay_pre = columns(heads, 1) * scale
    rate_row = jnp.broadcast_to(decay_rate[...], (heads, heads))
    diagonal = lax.broadcasted_iota(jnp.int32, (heads, heads), 0) == lax.broadcasted_iota(
        jnp.int32, (heads, heads), 1
    )
    rate_one = jnp.sum(jnp.where(diagonal, rate_row, 0.0), axis=1, keepdims=True)
    rates = jnp.concatenate([rate_one] * local, axis=0)
    softplus = jnp.maximum(decay_pre, 0.0) + jnp.log1p(jnp.exp(-jnp.abs(decay_pre)))
    decay = jnp.exp(-rates * softplus)
    beta_b = jnp.broadcast_to(beta, (pairs, size))
    decay_b = jnp.broadcast_to(decay, (pairs, size))

    pre = []
    for c in range(4):
        begin = pl.multiple_of(c * group * heads + deep * pairs, pairs)
        total = summed[pl.ds(begin, pairs), :]
        for k in range(1, outer):
            second[c, k].wait_recv()
            total = total + a2r[c, k].astype(f32)
        pre.append(total * scale)
    query = jax.nn.silu(pre[0])
    query = (
        query
        * lax.rsqrt(jnp.sum(query * query, axis=-1, keepdims=True) + norm_eps)
        * size ** (-0.5)
    )
    keyed = jax.nn.silu(pre[1])
    keyed = keyed * lax.rsqrt(jnp.sum(keyed * keyed, axis=-1, keepdims=True) + norm_eps)
    valued = jax.nn.silu(pre[2])
    turned = jnp.concatenate([keyed, query] * (128 // (2 * pairs)), axis=0).T
    load_state.wait()
    for r in range(local):
        for h in range(heads):
            i = r * heads + h
            key_col = turned[:, i : i + 1]
            query_col = turned[:, pairs + i : pairs + i + 1]
            old = state_v[r, h]
            decay_row = decay_b[i : i + 1]
            recalled = jnp.sum(key_col * old, axis=0, keepdims=True)
            write = beta_b[i : i + 1] * (valued[i : i + 1] - decay_row * recalled)
            new = decay_row * old + key_col * write
            new_state[r, h] = new
            read_v[i : i + 1, :] = jnp.sum(query_col * new, axis=0, keepdims=True)
    read = read_v[...]
    mixed = read * rms_scale(read) * head_gain[...] * jax.nn.silu(pre[3])
    mix_v[me] = mixed.astype(bf16)
    for k in range(1, n):
        start(
            remote(
                mix_v.at[me],
                mix_v.at[me],
                mx_s.at[k],
                mx_r.at[k],
                {"kv": lax.rem(me + k, n)},
            )
        )
    load_out.wait()
    for k in range(1, n):
        came = lax.rem(me + n - k, n)
        remote(
            mix_v.at[came], mix_v.at[came], mx_s.at[k], mx_r.at[k], {"kv": lax.rem(me + k, n)}
        ).wait_recv()
    for d in range(n):
        mix_f[d * pairs : (d + 1) * pairs, :] = mix_v[d].astype(f32)
    joined = jnp.concatenate(
        [mix_f[pl.ds(h, rows, stride=heads), :].astype(bf16) for h in range(heads)], axis=1
    )

    def over_tp(term, slots, send, recv):
        slots[tp] = term.astype(bf16)
        for k in range(1, n_tp):
            start(
                remote(
                    slots.at[tp],
                    slots.at[tp],
                    send.at[k],
                    recv.at[k],
                    {"tp": lax.rem(tp + k, n_tp)},
                )
            )
        for k in range(1, n_tp):
            came = lax.rem(tp + n_tp - k, n_tp)
            remote(
                slots.at[came],
                slots.at[came],
                send.at[k],
                recv.at[k],
                {"tp": lax.rem(tp + k, n_tp)},
            ).wait_recv()
        total = slots[0].astype(f32)
        for t in range(1, n_tp):
            total = total + slots[t].astype(f32)
        return total

    attended = over_tp(
        jnp.dot(joined, w_out_v[...], preferred_element_type=f32), t1, t1_s, t1_r
    )
    residual = (tok32 + attended).astype(bf16).astype(f32)
    gained_mid = (residual * mlp_gain[...]).astype(bf16)

    load_up.wait()
    ups = {}
    order = list(range(1, outer)) + [0]
    for step, j in enumerate(order):
        z = lax.rem(deep + j, outer)
        for k in list(range(1, inner)) + [0]:
            spot, device = plane_peer(k)
            begin = pl.multiple_of((spot * outer + z) * span, 128)
            term = jnp.dot(
                gained_mid, w_up_v[:, pl.ds(begin, span)], preferred_element_type=f32
            )
            u1[j, k] = term.astype(bf16)
            if k:
                ups[j, k] = start(
                    remote(u1.at[j, k], u1r.at[j, k], u1_s.at[j, k], u1_r.at[j, k], device)
                )
        if step == 0:
            squares = jnp.concatenate([residual * residual] * (128 // rows), axis=0)
            en[me] = lax.dot_general(
                jnp.ones((8, width), f32),
                squares,
                (((1,), (1,)), ((), ())),
                precision=lax.Precision.HIGHEST,
                preferred_element_type=f32,
            )
            for k in range(1, n):
                start(
                    remote(
                        en.at[me],
                        en.at[me],
                        en_s.at[k],
                        en_r.at[k],
                        {"kv": lax.rem(me + k, n)},
                    )
                )

    def plane_sum(j):
        total = u1[j, 0].astype(f32)
        for k in range(1, inner):
            ups[j, k].wait_recv()
            total = total + u1r[j, k].astype(f32)
        return total

    across = {}
    for j in range(1, outer):
        u2[j] = plane_sum(j).astype(bf16)
        _, device = deep_peer(j)
        across[j] = start(remote(u2.at[j], u2r.at[j], u2_s.at[j], u2_r.at[j], device))
    up = plane_sum(0)
    for k in range(1, n):
        came = lax.rem(me + n - k, n)
        remote(
            en.at[came], en.at[came], en_s.at[k], en_r.at[k], {"kv": lax.rem(me + k, n)}
        ).wait_recv()
    energy = en[0]
    for d in range(1, n):
        energy = energy + en[d]
    spread = jnp.broadcast_to(energy[0:1, :], (rows, 128))
    at_row = lax.broadcasted_iota(jnp.int32, (rows, 128), 0)
    energy_mid = jnp.sum(jnp.where(lanes == at_row, spread, 0.0), axis=1, keepdims=True)
    scale_mid = lax.rsqrt(energy_mid / total_width + norm_eps)
    for j in range(1, outer):
        across[j].wait_recv()
        up = up + u2r[j].astype(f32)
    mine = ours * outer + deep
    hid[mine] = jnp.square(jax.nn.relu(up * scale_mid)).astype(bf16)

    half = rows // 2
    flat = lax.rem(ours, 2)
    next_spot = (ours + 1 - 2 * flat, lax.rem(ours + 2, inner))
    corner = lax.rem(next_spot[0] + 2, inner)
    nearby = [{"kv": deep * inner + spot} for spot in next_spot]

    def block_of(spot, j):
        return spot * outer + lax.rem(deep + outer - j, outer)

    def near_copy(spot, j, side):
        block = hid.at[block_of(spot, j)]
        return remote(block, block, hp_s.at[j, side], hp_r.at[j, side], nearby[side])

    def corner_copy(spot, j, side):
        block = hid.at[block_of(spot, j), pl.ds((1 - side) * half, half)]
        return remote(block, block, hp_s.at[j, 2 + side], hp_r.at[j, 2 + side], nearby[side])

    def down(block):
        begin = pl.multiple_of(block * span, 128)
        return jnp.dot(
            hid[block], w_down_v[pl.ds(begin, span), :], preferred_element_type=f32
        )

    def pass_on(j):
        for side in range(2):
            near_copy(next_spot[side], j, side).wait_recv()
            start(corner_copy(next_spot[side], j, 1 - side))

    for side in range(2):
        start(near_copy(ours, 0, side))
    for k in range(1, outer):
        _, device = deep_peer(k)
        start(remote(hid.at[mine], hid.at[mine], hz_s.at[k], hz_r.at[k], device))
    load_down.wait()
    total = down(mine)
    for j in range(1, outer):
        block = block_of(ours, j)
        _, device = deep_peer(j)
        remote(hid.at[block], hid.at[block], hz_s.at[j], hz_r.at[j], device).wait_recv()
        for side in range(2):
            start(near_copy(ours, j, side))
        pass_on(j - 1)
        total = total + down(block)
    pass_on(outer - 1)
    for j in range(outer):
        for side in range(2):
            total = total + down(block_of(next_spot[side], j))
    for j in range(outer):
        for side in range(2):
            corner_copy(corner, j, side).wait_recv()
        total = total + down(block_of(corner, j))
    mixer = over_tp(total, t2, t2_s, t2_r)
    out[...] = (residual + mixer).astype(bf16)
    for copy in sent:
        copy.wait_send()


def write_back(out_v, state_v, out, state, sem):
    copies = [pltpu.make_async_copy(out_v, out, sem.at[0])]
    for r in range(state_v.shape[0]):
        copies.append(pltpu.make_async_copy(state_v.at[r], state.at[r], sem.at[1 + r]))
    for copy in copies:
        copy.start()
    for copy in copies:
        copy.wait()


def fused(n, n_tp, inner, *args):
    (
        tokens,
        mix_gain,
        w_query,
        w_key,
        w_value,
        w_gate,
        w_beta,
        w_decay,
        decay_rate,
        head_gain,
        state,
        w_out,
        mlp_gain,
        w_up,
        w_down,
    ) = args
    outer = n // inner
    rows, width = tokens.shape
    local, heads, size, _ = state.shape
    pairs = local * heads
    group = rows // inner
    span = w_up.shape[1] // n
    wide = heads * size
    pad = -(-local // 8) * 8
    hbm = pl.BlockSpec(memory_space=pltpu.HBM)
    vmem = pl.BlockSpec(memory_space=pltpu.VMEM)
    V = pltpu.VMEM
    S = pltpu.SemaphoreType.DMA
    pair = lambda *shape: [S(shape), S(shape)]
    scratch = [
        V((rows, width), bf16),
        V((1, width), f32),
        V((heads, width), bf16),
        V((heads, width), bf16),
        V((1, heads), f32),
        V((1, size), f32),
        V((1, width), f32),
        V((4, width, wide), bf16),
        V(state.shape, f32),
        V(w_out.shape, bf16),
        V(w_up.shape, bf16),
        V(w_down.shape, bf16),
        V((4, inner, group, wide), bf16),
        V((4, inner, group, wide), bf16),
        V((4 * group * heads, size), f32),
        V((4, outer, pairs, size), bf16),
        V((4, outer, pairs, size), bf16),
        V((inner, group, 128), f32),
        V((inner, group, 128), f32),
        V((group, 128), f32),
        V((outer, pad, 128), f32),
        V((outer, pad, 128), f32),
        V((pairs, size), f32),
        V((n, pairs, size), bf16),
        V((n * pairs, size), f32),
        V((n_tp, rows, width), bf16),
        V((outer, inner, rows, span), bf16),
        V((outer, inner, rows, span), bf16),
        V((outer, rows, span), bf16),
        V((outer, rows, span), bf16),
        V((n, 8, 128), f32),
        V((n, rows, span), bf16),
        V((n_tp, rows, width), bf16),
        S((7,)),
        S((7,)),
        S,
    ]
    for shape in (
        (4, inner),
        (inner,),
        (4, outer),
        (outer,),
        (n,),
        (n_tp,),
        (outer, inner),
        (outer,),
        (n,),
        (outer,),
        (outer, inner),
        (n_tp,),
    ):
        scratch += pair(*shape)
    held = pl.pallas_call(
        functools.partial(kernel, n, n_tp, inner),
        out_shape=(pltpu.VMEM((rows, width), bf16), pltpu.VMEM(state.shape, f32)),
        in_specs=[hbm] * 15,
        out_specs=(vmem, vmem),
        scratch_shapes=scratch,
        compiler_params=pltpu.CompilerParams(
            collective_id=0, has_side_effects=True, vmem_limit_bytes=60 * 1024 * 1024
        ),
    )(
        tokens,
        mix_gain.reshape(1, width),
        w_query,
        w_key,
        w_value,
        w_gate,
        w_beta.T,
        w_decay.T,
        decay_rate.reshape(1, heads),
        head_gain.reshape(1, size),
        state,
        w_out,
        mlp_gain.reshape(1, width),
        w_up,
        w_down,
    )
    return pl.pallas_call(
        write_back,
        out_shape=(
            jax.ShapeDtypeStruct((rows, width), bf16),
            jax.ShapeDtypeStruct(state.shape, f32),
        ),
        in_specs=[vmem, vmem],
        out_specs=(hbm, hbm),
        scratch_shapes=[S((1 + local,))],
    )(*[pltpu.with_memory_space_constraint(x, pltpu.VMEM) for x in held])


def solution(mesh):
    n, n_tp = mesh.shape["kv"], mesh.shape["tp"]
    inner = inner_size(n)

    def step(*args):
        if tiles(n, n_tp, inner, *args):
            return fused(n, n_tp, inner, *args)
        return body(*args)

    return jax.shard_map(
        step,
        mesh=mesh,
        in_specs=(
            P(None, "kv"),
            P("kv"),
            P("kv", "tp"),
            P("kv", "tp"),
            P("kv", "tp"),
            P("kv", "tp"),
            P("kv", "tp"),
            P("kv", "tp"),
            P("tp"),
            P(),
            P("kv", "tp", None, None),
            P("tp", "kv"),
            P("kv"),
            P("kv", "tp"),
            P("tp", "kv"),
        ),
        out_specs=(P(None, "kv"), P("kv", "tp", None, None)),
        check_vma=False,
    )
```
